768 devices in a mesh: sp: 16 (over y, core), tp: 48 (over z, x).
Axes of the slice: x: 4, y: 8, z: 12, core: 2. Of those that a mesh axis runs over, the one named last changes fastest.
Arguments:
- queries: bfloat16 [2048, 3072], P('sp'), may hold values from -6 to 6
- attn_out: bfloat16 [2048, 3072], P('sp'), may hold values from -3 to 3
- log_norm: float32 [2048, 12], P('sp'), as said below
- cotangent: bfloat16 [2048, 3072], P('sp'), may hold values from -96 to 96
- keys: bfloat16 [24576, 512], P(('sp', 'tp')), may hold values from -6 to 6
- values: bfloat16 [24576, 512], P(('sp', 'tp')), may hold values from -6 to 6
- source: bfloat16 [24576, 3072], P('sp', 'tp'), may hold values from -6 to 6
- w_query: bfloat16 [3072, 3072], P('tp'), may hold values from -0.109375 to 0.109375
- w_key: bfloat16 [3072, 512], P('tp'), may hold values from -0.109375 to 0.109375
- w_value: bfloat16 [3072, 512], P('tp'), may hold values from -0.109375 to 0.109375
Outputs:
- d_target: bfloat16 [2048, 3072], P('sp', 'tp')
- d_source: bfloat16 [24576, 3072], P('sp', 'tp')
- d_wvalue: float32 [3072, 512], P('tp')
The draws below stay inside these ranges and needn't reach their ends.
Inputs may be any that keep to these rules, and one draw needn't show every extreme that they name: `log_norm`: the logarithm of the softmax total saved by the forward pass, near log(24576) + 0.5.
All inputs are finite; a program needn't handle non-finite values.
Results may differ from the reference program's by a relative error of at most 0.024.
Values may be sent and summed in bfloat16 or wider, within the bound.
A program may use at most 32 MiB of HBM per device.

```python
import math
import jax
import jax.numpy as jnp
from jax import lax

HEADS = 12
KV_HEADS = 2
HEAD_DIM = 256
TARGET_ROWS_EACH = 128
D = 3072
KW = 512
TGT = 2048
SRC = 24576


def draw_log_norm(key, part):
    center = math.log(SRC) + 0.5
    spread = jax.random.uniform(key, (TGT, HEADS), jnp.float32, -0.5, 0.5)
    return (center + spread).astype(jnp.float32)


def level_of(key, dims, cuts, low, largest):
    def one(dim, blocks):
        heights = jax.random.uniform(jax.random.fold_in(jax.random.fold_in(key, 6), dim), (blocks,), jnp.float32, low / len(cuts), largest / len(cuts))
        return jnp.repeat(jnp.exp(heights), dims[dim] // blocks).reshape((-1,) + (1,) * (len(dims) - dim - 1))

    level = one(*cuts[0])
    for cut in cuts[1:]:
        level = level * one(*cut)
    return level


def scatter_about(own_key, extent, deviation, limit, shards=(), kind=jnp.bfloat16):
    factor_of = level_of(own_key, extent, shards, -0.22, 0.18) if shards else 1.0
    values = jax.random.normal(own_key, extent, jnp.float32) * deviation * factor_of
    return jnp.minimum(jnp.maximum(values, -limit), limit).astype(kind)


def setup_inputs(seed: int = 0) -> dict:
    splits = jax.random.split(jax.random.key(seed), 11)
    return {
        "queries": scatter_about(splits[0], (TGT, D), 1.0, 6.0, ((0, 16),)),
        "attn_out": scatter_about(splits[1], (TGT, D), 0.5, 3.0, ((0, 16),)),
        "log_norm": draw_log_norm(jax.random.fold_in(splits[10], 71), 0),
        "cotangent": scatter_about(splits[3], (TGT, D), 16.0, 96.0, ((0, 16),)),
        "keys": scatter_about(splits[4], (SRC, KW), 1.0, 6.0, ((0, 768),)),
        "values": scatter_about(splits[5], (SRC, KW), 1.0, 6.0, ((0, 768),)),
        "source": scatter_about(splits[6], (SRC, D), 1.0, 6.0, ((0, 16), (1, 48))),
        "w_query": scatter_about(splits[7], (D, D), D ** -0.5, 0.109375, ((0, 48),)),
        "w_key": scatter_about(splits[8], (D, KW), D ** -0.5, 0.109375, ((0, 48),)),
        "w_value": scatter_about(splits[9], (D, KW), D ** -0.5, 0.109375, ((0, 48),)),
    }


def reference(queries, attn_out, log_norm, cotangent, keys, values, source, w_query, w_key, w_value):
    single_precision = jnp.float32
    repeat = HEADS // KV_HEADS
    score_scale = 1.0 / math.sqrt(HEAD_DIM)
    src_rows = keys.shape[0]
    shared_key_heads = keys.astype(single_precision).reshape(src_rows, KV_HEADS, HEAD_DIM)
    shared_value_heads = values.astype(single_precision).reshape(src_rows, KV_HEADS, HEAD_DIM)
    blocks = queries.shape[0] // TARGET_ROWS_EACH

    def step(carry, index):
        dk_total, dv_total = carry
        start = index * TARGET_ROWS_EACH

        def rows(array):
            return lax.dynamic_slice_in_dim(array, start, TARGET_ROWS_EACH, 0)
        query_tensor4 = rows(queries).astype(single_precision).reshape(TARGET_ROWS_EACH, KV_HEADS, repeat, HEAD_DIM)
        output_gradient4 = rows(cotangent).astype(single_precision).reshape(TARGET_ROWS_EACH, KV_HEADS, repeat, HEAD_DIM)
        out4 = rows(attn_out).astype(single_precision).reshape(TARGET_ROWS_EACH, KV_HEADS, repeat, HEAD_DIM)
        lse = jnp.transpose(rows(log_norm).reshape(TARGET_ROWS_EACH, KV_HEADS, repeat), (1, 2, 0))[..., None]
        delta = jnp.transpose(lax.optimization_barrier(jnp.sum(output_gradient4 * out4, axis=3)), (1, 2, 0))[..., None]
        logit_scores = jnp.einsum('znjk,wnk->njzw', query_tensor4, shared_key_heads) * score_scale
        probs = jnp.exp(logit_scores - lse)
        probabilities16 = lax.optimization_barrier(probs.astype(jnp.bfloat16)).astype(single_precision)
        prob_gradient = jnp.einsum('znjk,wnk->njzw', output_gradient4, shared_value_heads)
        score_gradient = lax.optimization_barrier((probs * (prob_gradient - delta)).astype(jnp.bfloat16)).astype(single_precision)
        query_gradient = (jnp.einsum('wohn,nwb->hwob', score_gradient, shared_key_heads) * score_scale).reshape(TARGET_ROWS_EACH, -1)
        key_gradient = jnp.einsum('nkjv,jnka->vna', score_gradient, query_tensor4) * score_scale
        value_gradient = jnp.einsum('nkjv,jnka->vna', probabilities16, output_gradient4)
        dk16 = lax.optimization_barrier(key_gradient.reshape(src_rows, -1).astype(jnp.bfloat16)).astype(single_precision)
        dv16 = lax.optimization_barrier(value_gradient.reshape(src_rows, -1).astype(jnp.bfloat16)).astype(single_precision)
        return ((dk_total + dk16, dv_total + dv16), query_gradient.astype(jnp.bfloat16))
    start_carry = (jnp.zeros((src_rows, KW), single_precision), jnp.zeros((src_rows, KW), single_precision))
    (dk_total, dv_total), dq_blocks = lax.scan(step, start_carry, jnp.arange(blocks, dtype=jnp.int32))
    dq16 = dq_blocks.reshape(queries.shape[0], -1)
    d_target = jnp.dot(dq16, w_query.T, preferred_element_type=single_precision).astype(jnp.bfloat16)
    stacked = jnp.concatenate([dk_total.astype(jnp.bfloat16), dv_total.astype(jnp.bfloat16)], axis=1)
    weights = jnp.concatenate([w_key, w_value], axis=1)
    d_source = jnp.dot(stacked, weights.T, preferred_element_type=single_precision).astype(jnp.bfloat16)
    d_wvalue = jnp.dot(source.T, dv_total.astype(jnp.bfloat16), preferred_element_type=single_precision)
    return (d_target, d_source, d_wvalue)
```

```python
import math

import jax
import jax.numpy as jnp
from jax import lax
from jax.experimental import pallas as pl
from jax.experimental.pallas import tpu as pltpu
from jax.sharding import Mesh
from jax.sharding import PartitionSpec as P

HEADS = 12
KV_HEADS = 2
HEAD_DIM = 256
PER_GROUP = HEADS // KV_HEADS
NY, NC, NZ, NX = 8, 2, 12, 4
MESH = pl.DeviceIdType.MESH
F32 = jnp.float32
BF16 = jnp.bfloat16
NT = (((1,), (1,)), ((), ()))
TN = (((0,), (0,)), ((), ()))
NN = (((1,), (0,)), ((), ()))
Y_CHAINS = ((0, 1, 4), (1, -1, 4), (1, 1, 3), (0, -1, 3))
Z_CHAINS = ((0, 1, 6), (1, -1, 6), (1, 1, 5), (0, -1, 5))
COPIES = 176


def mm(a, b, dims):
    return lax.dot_general(a, b, dims, preferred_element_type=F32)


def kernel(
    q_ref, o_ref, do_ref, lse_ref, kv_ref, src_ref, wkv_ref, wq_ref,
    dt_ref, ds_ref, dw_ref,
    kv, qs, dos, delta, dq_acc, part, from_core, paired, ring_in, ring_out, own,
    dqp, x_in, x_sum, z_in, chunk, gathered, dq_all,
    wkv, wq, sx, wvp, wv_in, sums, sum_in, total, totals,
    dst_part, dst_in, dtp, dt_in,
    send_sem, recv_sem,
):
    y, c, z, x = (lax.axis_index(a) for a in ("y", "c", "z", "x"))
    scale = 1.0 / math.sqrt(HEAD_DIM)
    made = []

    def step(v, d, n):
        return lax.rem(v + d + n, n)

    def remote(src, dst, **where):
        number = len(made)
        copy = pltpu.make_async_remote_copy(
            src_ref=src,
            dst_ref=dst,
            send_sem=send_sem.at[number],
            recv_sem=recv_sem.at[number],
            device_id=where,
            device_id_type=MESH,
        )
        copy.start()
        made.append(copy)
        return copy

    barrier = pltpu.get_barrier_semaphore()
    peers = [{"y": step(y, 1, NY)}, {"y": step(y, -1, NY)}, {"c": 1 - c}]
    peers += [{"x": step(x, d, NX)} for d in range(1, NX)]
    peers += [{"z": step(z, d, NZ)} for d in range(1, NZ)]
    for peer in peers:
        pl.semaphore_signal(barrier, inc=1, device_id=peer, device_id_type=MESH)
    pl.semaphore_wait(barrier, len(peers))

    hops = {}
    for n, (w, d, length) in enumerate(Y_CHAINS):
        hops[n] = remote(kv_ref.at[w], kv.at[y, c, w], y=step(y, d, NY))
    to_core = [remote(kv_ref.at[w], kv.at[y, c, w], c=1 - c) for w in range(2)]
    x_src = [remote(src_ref.at[:, step(x, d, NX)], sx.at[x], x=step(x, d, NX)) for d in range(1, NX)]
    x_wkv = [remote(wkv_ref.at[c], wkv.at[x, c], x=step(x, d, NX)) for d in range(1, NX)]

    kv[y, c] = kv_ref[...]
    wkv[x] = wkv_ref[...]
    wq[x] = wq_ref[...]
    for xx in range(NX):
        @pl.when(x == xx)
        def _():
            sx[xx] = src_ref[:, xx]
    for g in range(KV_HEADS):
        for h in range(PER_GROUP):
            columns = slice((g * PER_GROUP + h) * HEAD_DIM, (g * PER_GROUP + h + 1) * HEAD_DIM)
            rows = slice(h * 128, (h + 1) * 128)
            qs[g, rows] = q_ref[:, columns]
            dos[g, rows] = do_ref[:, columns]
            prod = do_ref[:, columns].astype(F32) * o_ref[:, columns].astype(F32)
            halves = prod[:, :128] + prod[:, 128:]
            delta[g, :, rows] = jnp.sum(jnp.transpose(halves), axis=0, keepdims=True)

    for h in range(1, 5):
        for n, (w, d, length) in enumerate(Y_CHAINS):
            if h > length:
                continue
            hops[n].wait_recv()
            at = kv.at[step(y, -d * h, NY), c, w]
            if h < length:
                hops[n] = remote(at, at, y=step(y, d, NY))
            to_core.append(remote(at, at, c=1 - c))
    for copy in to_core:
        copy.wait_recv()

    ROWS = 256
    for g in range(KV_HEADS):
        cols = slice(g * HEAD_DIM, (g + 1) * HEAD_DIM)

        def block(n, carry, g=g, cols=cols):
            base = n * (ROWS // 64)
            kb = kv[pl.ds(base, ROWS // 64), :, 0, :, cols].reshape(ROWS, HEAD_DIM)
            vb = kv[pl.ds(base, ROWS // 64), :, 1, :, cols].reshape(ROWS, HEAD_DIM)
            scores = mm(kb, qs[g], NT) * scale
            probs = jnp.exp(scores - lse_ref[g])
            dprob = mm(vb, dos[g], NT)
            dscore = (probs * (dprob - delta[g])).astype(BF16)
            dk = (mm(dscore, qs[g], NN) * scale).astype(BF16)
            dv = mm(probs.astype(BF16), dos[g], NN).astype(BF16)
            term = mm(dscore, kb, TN) * scale
            dq_acc[g] = jnp.where(n == 0, term, dq_acc[g] + term)
            for yy in range(ROWS // 64):
                for cc in range(NC):
                    at = slice((yy * 2 + cc) * 32, (yy * 2 + cc + 1) * 32)
                    part[cc, base + yy, 0, :, cols] = dk[at]
                    part[cc, base + yy, 1, :, cols] = dv[at]
            return carry

        lax.fori_loop(0, 512 // ROWS, block, 0)
    for g in range(KV_HEADS):
        for h in range(PER_GROUP):
            for xx in range(NX):
                at = h * 128 + xx * 32
                dqp[xx, g * PER_GROUP + h] = dq_acc[g, at : at + 32].astype(BF16)

    order = (4, 3, -3, 2, -2, 1, -1, 0)
    core_in = {d: remote(part.at[1 - c, step(y, d, NY)], from_core.at[step(y, d, NY)], c=1 - c) for d in order}
    x_dq = [remote(dqp.at[step(x, d, NX)], x_in.at[d - 1], x=step(x, d, NX)) for d in range(1, NX)]
    x_wq = [remote(wq_ref.at[c], wq.at[x, c], x=step(x, d, NX)) for d in range(1, NX)]
    for d in range(1, NX):
        x_wkv[d - 1].wait_recv()
    c_wkv = [remote(wkv.at[step(x, -d, NX), c], wkv.at[step(x, -d, NX), c], c=1 - c) for d in range(1, NX)]

    for d in order:
        core_in[d].wait_recv()
        at = step(y, d, NY)
        paired[at] = (part[c, at].astype(F32) + from_core[at].astype(F32)).astype(BF16)

    for n, (w, d, length) in enumerate(Y_CHAINS):
        hops[n] = remote(paired.at[step(y, d * length, NY), w], ring_in.at[n, 0], y=step(y, d, NY))

    def sum_over_x():
        for d in range(1, NX):
            x_dq[d - 1].wait_recv()
        for hh in range(NZ):
            total_rows = dqp[x, hh].astype(F32)
            for d in range(1, NX):
                total_rows += x_in[d - 1, hh].astype(F32)
            x_sum[hh] = total_rows.astype(BF16)
        return [remote(x_sum.at[step(z, d, NZ)], z_in.at[d - 1], z=step(z, d, NZ)) for d in range(1, NZ)]

    for h in range(1, 5):
        for n, (w, d, length) in enumerate(Y_CHAINS):
            if h > length:
                continue
            hops[n].wait_recv()
            if h < length:
                ring_out[n, h - 1] = (
                    ring_in[n, h - 1].astype(F32) + paired[step(y, d * (length - h), NY), w].astype(F32)
                ).astype(BF16)
                hops[n] = remote(ring_out.at[n, h - 1], ring_in.at[n, h], y=step(y, d, NY))
        if h == 3:
            z_dq = sum_over_x()
    last = {(w, d): ring_in.at[n, length - 1] for n, (w, d, length) in enumerate(Y_CHAINS)}
    for w in range(2):
        own[w] = (
            paired[y, w].astype(F32) + last[w, 1][...].astype(F32) + last[w, -1][...].astype(F32)
        ).astype(BF16)

    for n, (w, d, length) in enumerate(Z_CHAINS):
        hops[n] = remote(own.at[w], gathered.at[w, z], z=step(z, d, NZ))
    for w in range(2):
        gathered[w, z] = own[w]

    def over_z(h):
        for n, (w, d, length) in enumerate(Z_CHAINS):
            if h > length:
                continue
            hops[n].wait_recv()
            if h < length:
                at = gathered.at[w, step(z, -d * h, NZ)]
                hops[n] = remote(at, at, z=step(z, d, NZ))

    over_z(1)
    over_z(2)
    for copy in z_dq:
        copy.wait_recv()
    rows32 = x_sum[z].astype(F32)
    for d in range(1, NZ):
        rows32 += z_in[d - 1].astype(F32)
    chunk[...] = rows32.astype(BF16)
    z_dq_all = [remote(chunk, dq_all.at[z], z=step(z, d, NZ)) for d in range(1, NZ)]
    dq_all[z] = chunk[...]
    over_z(3)
    over_z(4)
    for d in range(1, NX):
        x_wq[d - 1].wait_recv()
    c_wq = [remote(wq.at[step(x, -d, NX), c], wq.at[step(x, -d, NX), c], c=1 - c) for d in range(1, NX)]
    over_z(5)
    over_z(6)

    dv_rows = gathered[1].reshape(NZ * 32, 512)
    for d in range(1, NX):
        x_src[d - 1].wait_recv()
    for xx in range(NX):
        wvp[xx] = mm(sx[xx].reshape(NZ * 32, 64), dv_rows, TN).astype(BF16)
    x_wv = [remote(wvp.at[step(x, d, NX)], wv_in.at[d - 1], x=step(x, d, NX)) for d in range(1, NX)]
    for d in range(1, NX):
        c_wkv[d - 1].wait_recv()
    dk_rows = gathered[0].reshape(NZ * 32, 512)
    weights = wkv[...]
    w_key = weights[:, :, 0].reshape(NX * 64, 512)
    w_value = weights[:, :, 1].reshape(NX * 64, 512)
    grad = mm(w_key, dk_rows, NT) + mm(w_value, dv_rows, NT)
    for xx in range(NX):
        dst_part[xx] = grad[xx * 64 : (xx + 1) * 64].astype(BF16)
    x_ds = [remote(dst_part.at[step(x, d, NX)], dst_in.at[x], x=step(x, d, NX)) for d in range(1, NX)]
    dst_in[x] = dst_part[x]

    for copy in x_wv:
        copy.wait_recv()
    w_sum = wvp[x].astype(F32)
    for d in range(1, NX):
        w_sum += wv_in[d - 1].astype(F32)
    for j in range(16):
        sums[j] = w_sum[(j // 4) * 16 : (j // 4 + 1) * 16, (j % 4) * 128 : (j % 4 + 1) * 128].astype(BF16)
    others = [(dy, dc) for dy in range(NY) for dc in range(NC) if dy or dc]

    def sp_peer(dy, dc):
        py, pc = step(y, dy, NY), lax.rem(c + dc, NC)
        return py, pc, py * NC + pc

    sp_sum = []
    for n, (dy, dc) in enumerate(others):
        py, pc, number = sp_peer(dy, dc)
        sp_sum.append(remote(sums.at[number], sum_in.at[n], y=py, c=pc))

    for copy in z_dq_all:
        copy.wait_recv()
    for copy in c_wq:
        copy.wait_recv()
    out = jnp.zeros((32, NX * 64), F32)
    for zz in range(NZ):
        cols = slice(zz * HEAD_DIM, (zz + 1) * HEAD_DIM)
        out += mm(dq_all[zz], wq[:, :, :, cols].reshape(NX * 64, HEAD_DIM), NT)
    for half in range(2):
        dtp[half] = out[:, half * 128 : (half + 1) * 128].astype(BF16)
    x_dt = [
        remote(dtp.at[step(x, d, NX) // 2], dt_in.at[x], x=step(x, d, NX)) for d in range(1, NX)
    ]
    dt_in[x] = dtp[x // 2]

    for copy in sp_sum:
        copy.wait_recv()
    own_sum = sums[y * NC + c].astype(F32)
    for n in range(len(others)):
        own_sum += sum_in[n].astype(F32)
    total[...] = own_sum
    sp_all = []
    for dy, dc in others:
        py, pc, number = sp_peer(dy, dc)
        sp_all.append(remote(total, totals.at[y * NC + c], y=py, c=pc))
    totals[y * NC + c] = own_sum

    for copy in x_ds:
        copy.wait_recv()
    for xx in range(NX):
        rows = jnp.transpose(dst_in[xx].astype(F32)).astype(BF16)
        ds_ref[:, xx] = rows.reshape(NZ, 32, 64)
    for copy in x_dt:
        copy.wait_recv()
    odd = lax.rem(x, 2) == 1
    for xx in range(NX):
        both = dt_in[xx]
        dt_ref[xx * 32 : (xx + 1) * 32] = jnp.where(odd, both[:, 64:], both[:, :64])
    for copy in sp_all:
        copy.wait_recv()
    for j in range(16):
        dw_ref[(j // 4) * 16 : (j // 4 + 1) * 16, (j % 4) * 128 : (j % 4 + 1) * 128] = totals[j]
    for copy in made:
        copy.wait_send()


def shards(queries, attn_out, log_norm, cotangent, keys, values, source, w_query, w_key, w_value):
    lse = jnp.transpose(log_norm).reshape(KV_HEADS, 1, PER_GROUP * 128)
    kv = jnp.stack([keys, values])
    wkv = jnp.stack([w_key.reshape(2, 32, 512), w_value.reshape(2, 32, 512)], axis=1)
    vmem = pl.BlockSpec(memory_space=pltpu.VMEM)

    def bf(*shape):
        return pltpu.VMEM(shape, BF16)

    def f32(*shape):
        return pltpu.VMEM(shape, F32)

    d_target, d_source, d_wvalue = pl.pallas_call(
        kernel,
        out_shape=(
            jax.ShapeDtypeStruct((128, 64), BF16),
            jax.ShapeDtypeStruct((NZ, NX, 32, 64), BF16),
            jax.ShapeDtypeStruct((64, 512), F32),
        ),
        in_specs=[vmem] * 8,
        out_specs=(vmem,) * 3,
        scratch_shapes=[
            bf(NY, NC, 2, 32, 512),
            bf(2, 768, 256), bf(2, 768, 256), f32(2, 1, 768), f32(2, 768, 256),
            bf(NC, NY, 2, 32, 512), bf(NY, 2, 32, 512), bf(NY, 2, 32, 512),
            bf(4, 4, 32, 512), bf(4, 3, 32, 512), bf(2, 32, 512),
            bf(NX, NZ, 32, 256), bf(NX - 1, NZ, 32, 256), bf(NZ, 32, 256),
            bf(NZ - 1, 32, 256), bf(32, 256), bf(2, NZ, 32, 512), bf(NZ, 32, 256),
            bf(NX, 2, 2, 32, 512), bf(NX, 2, 32, 3072), bf(NX, NZ, 32, 64),
            bf(NX, 64, 512), bf(NX - 1, 64, 512), bf(16, 16, 128), bf(15, 16, 128),
            f32(16, 128), f32(16, 16, 128),
            bf(NX, 64, 384), bf(NX, 64, 384), bf(2, 32, 128), bf(NX, 32, 128),
            pltpu.SemaphoreType.DMA((COPIES,)), pltpu.SemaphoreType.DMA((COPIES,)),
        ],
        compiler_params=pltpu.CompilerParams(
            collective_id=0, has_side_effects=True, vmem_limit_bytes=56 * 2**20
        ),
    )(
        queries, attn_out, cotangent, lse, kv, source.reshape(NZ, NX, 32, 64), wkv,
        w_query.reshape(2, 32, 3072),
    )
    return d_target, d_source.reshape(1536, 64), d_wvalue


def solution(mesh):
    split = Mesh(mesh.devices.reshape(NY, NC, NZ, NX), ("y", "c", "z", "x"))
    sp, tp = ("y", "c"), ("z", "x")
    every = sp + tp
    in_specs = (
        P(sp, None), P(sp, None), P(sp, None), P(sp, None),
        P(every, None), P(every, None), P(sp, tp),
        P(tp, None), P(tp, None), P(tp, None),
    )
    out_specs = (P(sp, tp), P(sp, tp), P(tp, None))
    return jax.shard_map(
        shards, mesh=split, in_specs=in_specs, out_specs=out_specs, check_vma=False
    )
```

```python
import math

import jax
import jax.numpy as jnp
from jax import lax
from jax.experimental import pallas as pl
from jax.experimental.pallas import tpu as pltpu
from jax.sharding import Mesh
from jax.sharding import PartitionSpec as P

HEADS = 12
KV_HEADS = 2
HEAD_DIM = 256
PER_GROUP = HEADS // KV_HEADS
NY, NC, NZ, NX = 8, 2, 12, 4
MESH = pl.DeviceIdType.MESH
F32 = jnp.float32
BF16 = jnp.bfloat16
NT = (((1,), (1,)), ((), ()))
TN = (((0,), (0,)), ((), ()))
NN = (((1,), (0,)), ((), ()))
Y_CHAINS = ((0, 1, 4), (1, -1, 4), (1, 1, 3), (0, -1, 3))
Z_CHAINS = ((0, 1, 6), (1, -1, 6), (1, 1, 5), (0, -1, 5))
DQ_CHAINS = ((None, 1, 6), (None, -1, 5))
Y_JUMP, Z_JUMP = 2, 2
NEAR, FAR = (0, 1, -1, 2), (4, 3, -3, -2)
COPIES, SENDS = 182, 64


def mm(a, b, dims):
    return lax.dot_general(a, b, dims, preferred_element_type=F32)


def kernel(
    q_hbm, o_hbm, do_hbm, lse_hbm, k_hbm, v_hbm, src_hbm, wk_hbm, wv_hbm, wq_hbm,
    dt_ref, ds_ref, dw_ref,
    q_ref, o_ref, do_ref, lse_ref, src_ref,
    kv, qs, dos, delta, lse, dq_acc, part, from_core, paired, ring_in, ring_out, own,
    dqp, x_in, x_sum, z_in, z_out, chunk, gathered, dq_all,
    wkv, wq, sxo, sx, wvp, wv_core, wv_half, wv_in, sums, sum_in, total, totals,
    dst_part, dst_in, ds_rows, dtp, dt_in,
    z_sem, local_sem, send_sem, recv_sem,
):
    y, c, z, x = (lax.axis_index(a) for a in ("y", "c", "z", "x"))
    scale = 1.0 / math.sqrt(HEAD_DIM)
    made = []

    def step(v, d, n):
        return lax.rem(v + d + n, n)

    def remote(src, dst, **where):
        number = len(made)
        if number >= SENDS:
            made[number - SENDS].wait_send()
        copy = pltpu.make_async_remote_copy(
            src_ref=src,
            dst_ref=dst,
            send_sem=send_sem.at[number % SENDS],
            recv_sem=recv_sem.at[number],
            device_id=where,
            device_id_type=MESH,
        )
        copy.start()
        made.append(copy)
        return copy

    def spread(copies, name, axis, here, size, d, length, jump, at, t):
        if t:
            copies[name, t].wait_recv()
        if t % jump == 0:
            for far in range(min(jump, length - t), 0, -1):
                src, dst = at(t)
                copies[name, t + far] = remote(src, dst, **{axis: step(here, d * far, size)})

    here = {}

    def load(name, src, dst):
        here[name] = pltpu.make_async_copy(src, dst, local_sem.at[len(here)])
        here[name].start()

    load("v", v_hbm, kv.at[y, c, :, 1])
    load("k", k_hbm, kv.at[y, c, :, 0])
    load("wk", wk_hbm, wkv.at[x, :, 0])
    load("wv", wv_hbm, wkv.at[x, :, 1])
    load("src", src_hbm, src_ref)
    load("q", q_hbm, q_ref)
    load("do", do_hbm, do_ref)
    load("o", o_hbm, o_ref)
    load("lse", lse_hbm, lse_ref)
    load("wq", wq_hbm, wq.at[x])

    barrier = pltpu.get_barrier_semaphore()
    peers = [{"y": step(y, d, NY)} for d in (1, -1, 2, -2)] + [{"c": 1 - c}]
    peers += [{"x": step(x, d, NX)} for d in range(1, NX)]
    peers += [{"z": step(z, 1, NZ)}, {"z": step(z, -1, NZ)}]
    for peer in peers:
        pl.semaphore_signal(barrier, inc=1, device_id=peer, device_id_type=MESH)
    here["k"].wait()
    here["v"].wait()
    pl.semaphore_wait(barrier, len(peers))

    def z_tell(number, far):
        for n, d in enumerate((1, -1)):
            pl.semaphore_signal(z_sem.at[number, n], inc=1, device_id={"z": step(z, d * far, NZ)}, device_id_type=MESH)

    def z_hear(number):
        for n in range(2):
            pl.semaphore_wait(z_sem.at[number, n], 1)

    z_tell(0, 1)
    hops = {}
    ways = {}
    core_kv = {}

    def kv_spread(t):
        for r, d, length in Y_CHAINS:
            if t > length:
                continue
            block = kv.at[step(y, -d * t, NY), c, r]
            spread(ways, (r, d), "y", y, NY, d, length, Y_JUMP, lambda t: (block, block), t)
            if t:
                core_kv[4 if t == 4 else -d * t, r] = remote(block, block, c=1 - c)

    kv_spread(0)
    core_kv[0] = remote(kv.at[y, c], kv.at[y, c], c=1 - c)
    here["wk"].wait()
    here["wv"].wait()
    x_wkv = [remote(wkv.at[x, c], wkv.at[x, c], x=step(x, d, NX)) for d in range(1, NX)]
    here["src"].wait()
    for zz in range(NZ):
        rows = jnp.transpose(src_ref[:, zz * 128 : (zz + 1) * 128].astype(F32)).astype(BF16)
        for xx in range(NX):
            sxo[xx, zz] = rows[xx * 32 : (xx + 1) * 32]
    x_src = [remote(sxo.at[step(x, d, NX)], sx.at[x], x=step(x, d, NX)) for d in range(1, NX)]

    for name in ("q", "do", "o", "lse"):
        here[name].wait()

    def prepare(g):
        for h in range(PER_GROUP):
            head = g * PER_GROUP + h
            columns = slice(head * HEAD_DIM, (head + 1) * HEAD_DIM)
            rows = slice(h * 128, (h + 1) * 128)
            qs[g, rows] = q_ref[:, columns]
            dos[g, rows] = do_ref[:, columns]
            prod = do_ref[:, columns].astype(F32) * o_ref[:, columns].astype(F32)
            halves = prod[:, :128] + prod[:, 128:]
            delta[g, :, rows] = jnp.sum(jnp.transpose(halves), axis=0, keepdims=True)
            lse[g, :, rows] = lse_ref[head : head + 1]

    def attend(offsets, first):
        for d in offsets:
            for r in range(2):
                if (d, r) in core_kv:
                    core_kv[d, r].wait_recv()
        if first:
            core_kv[0].wait_recv()
        places = [(d, lax.rem(c + dc, NC)) for d in offsets for dc in range(NC)]
        for g in range(KV_HEADS):
            cols = slice(g * HEAD_DIM, (g + 1) * HEAD_DIM)

            def rows_of(w):
                return jnp.concatenate(
                    [kv[step(y, d, NY), cc, :, w, :, cols].reshape(32, HEAD_DIM) for d, cc in places], axis=0
                )

            kb, vb = rows_of(0), rows_of(1)
            scores = mm(kb, qs[g], NT) * scale
            probs = jnp.exp(scores - lse[g])
            dprob = mm(vb, dos[g], NT)
            dscore = (probs * (dprob - delta[g])).astype(BF16)
            dk = (mm(dscore, qs[g], NN) * scale).astype(BF16)
            dv = mm(probs.astype(BF16), dos[g], NN).astype(BF16)
            term = mm(dscore, kb, TN) * scale
            at = slice(g * 768, (g + 1) * 768)
            dq_acc[at] = term if first else dq_acc[at] + term
            for n, (d, cc) in enumerate(places):
                rows = slice(n * 32, n * 32 + 32)
                part[cc, step(y, d, NY), :, 0, :, cols] = dk[rows].reshape(2, 16, HEAD_DIM)
                part[cc, step(y, d, NY), :, 1, :, cols] = dv[rows].reshape(2, 16, HEAD_DIM)

    core_in = {}

    def to_core(offsets):
        for d in offsets:
            at = step(y, d, NY)
            core_in[d] = remote(part.at[1 - c, at], from_core.at[at], c=1 - c)

    def pair(offsets):
        for d in offsets:
            core_in[d].wait_recv()
            at = step(y, d, NY)
            paired[at] = (part[c, at].astype(F32) + from_core[at].astype(F32)).astype(BF16)

    prepare(0)
    kv_spread(1)
    z_hear(0)
    z_tell(1, 2)
    prepare(1)
    kv_spread(2)
    attend(NEAR, True)
    to_core(NEAR)
    z_hear(1)
    z_tell(2, 2)
    kv_spread(3)
    kv_spread(4)
    pair(NEAR)
    attend(FAR, False)

    to_core(FAR)
    x_dq = {}
    for m in range(6):
        for s, d in enumerate((6 - m, m - 5)):
            for xx in range(NX):
                at = pl.multiple_of(step(z, d, NZ) * 128 + xx * 32, 32)
                dqp[xx, m, s] = dq_acc[pl.ds(at, 32)].astype(BF16)
        for d in range(1, NX):
            x_dq[m, d] = remote(dqp.at[step(x, d, NX), m], x_in.at[d - 1, m], x=step(x, d, NX))
    here["wq"].wait()
    x_wq = [remote(wq.at[x, c], wq.at[x, c], x=step(x, d, NX)) for d in range(1, NX)]

    pair(FAR)
    y_sent = {}

    def y_send(r, d, length, t, value_ref):
        far = 2 - t % 2
        n = Y_CHAINS.index((r, d, length))
        y_sent[r, d, t] = remote(value_ref, ring_in.at[n, t - 1], y=step(y, d * far, NY))

    for t in (4, 3):
        for r, d, length in Y_CHAINS:
            if t <= length:
                y_send(r, d, length, t, paired.at[step(y, d * t, NY), r])
    for r, d, length in Y_CHAINS:
        y_send(r, d, length, 1, paired.at[step(y, d, NY), r])

    def y_middle():
        for n, (r, d, length) in enumerate(Y_CHAINS):
            rows = paired[step(y, d * 2, NY), r].astype(F32)
            for t in range(3, length + 1):
                y_sent[r, d, t].wait_recv()
                rows += ring_in[n, t - 1].astype(F32)
            ring_out[n] = rows.astype(BF16)
            y_send(r, d, length, 2, ring_out.at[n])

    z_dq = []

    def dq_part(m):
        for d in range(1, NX):
            x_dq[m, d].wait_recv()
        rows = dqp[x, m].astype(F32)
        for d in range(1, NX):
            rows += x_in[d - 1, m].astype(F32)
        for s, d in enumerate((6 - m, m - 5)):
            if d:
                z_out[s, m] = rows[s].astype(BF16)
                z_dq.append((s, m, remote(z_out.at[s, m], z_in.at[s, m], z=step(z, d, NZ))))
            else:
                x_sum[...] = rows[s]

    z_hear(2)
    dq_part(0)
    y_middle()
    for m in range(1, 4):
        dq_part(m)
    for r in range(2):
        rows = paired[y, r].astype(F32)
        for n, (r_, d, length) in enumerate(Y_CHAINS):
            if r_ == r:
                for t in (1, 2):
                    y_sent[r, d, t].wait_recv()
                    rows += ring_in[n, t - 1].astype(F32)
        for w in range(2):
            own[w, r] = rows[w].astype(BF16)

    def over_z(w, t):
        for r, d, length in Z_CHAINS:
            if t > length:
                continue
            at = step(z, -d * t, NZ)
            block = gathered.at[w, at, r]
            src = block if t else own.at[w, r]
            spread(ways, (w, r, d), "z", z, NZ, d, length, Z_JUMP, lambda t: (src, block), t)

    def dq_over_z(t):
        for _, d, length in DQ_CHAINS:
            if t > length:
                continue
            block = dq_all.at[step(z, -d * t, NZ)]
            src = block if t else chunk
            spread(ways, ("dq", d), "z", z, NZ, d, length, Z_JUMP, lambda t: (src, block), t)

    over_z(1, 0)
    for w in range(2):
        gathered[w, z] = own[w]
    dq_part(4)
    dq_part(5)
    for d in range(1, NX):
        x_wkv[d - 1].wait_recv()
    c_wkv = [remote(wkv.at[step(x, -d, NX), c], wkv.at[step(x, -d, NX), c], c=1 - c) for d in range(1, NX)]
    for copy in x_src:
        copy.wait_recv()
    sx[x] = sxo[x]
    over_z(1, 1)
    over_z(1, 2)
    over_z(0, 0)
    dq_rows = x_sum[...]
    for s, m, copy in z_dq:
        copy.wait_recv()
        dq_rows += z_in[s, m].astype(F32)
    chunk[...] = dq_rows.astype(BF16)
    dq_over_z(0)
    dq_all[z] = chunk[...]
    over_z(1, 3)
    over_z(1, 4)
    over_z(0, 1)
    over_z(0, 2)
    dq_over_z(1)
    dq_over_z(2)
    over_z(1, 5)
    over_z(1, 6)

    dv_rows = gathered[1].reshape(NZ * 32, 512)
    for xx in range(NX):
        term = mm(sx[xx].reshape(NZ * 32, 64), dv_rows, TN).astype(BF16)
        for half in range(2):
            wvp[half, xx] = term[:, half * 256 : (half + 1) * 256]
    core_wv = remote(wvp.at[1 - c], wv_core, c=1 - c)
    over_z(0, 3)
    over_z(0, 4)
    core_wv.wait_recv()
    wv_half[...] = (wvp[c].astype(F32) + wv_core[...].astype(F32)).astype(BF16)
    x_wv = [remote(wv_half.at[step(x, d, NX)], wv_in.at[d - 1], x=step(x, d, NX)) for d in range(1, NX)]
    dq_over_z(3)
    dq_over_z(4)
    for d in range(1, NX):
        x_wq[d - 1].wait_recv()
    c_wq = [remote(wq.at[step(x, -d, NX), c], wq.at[step(x, -d, NX), c], c=1 - c) for d in range(1, NX)]
    for copy in x_wv:
        copy.wait_recv()
    w_sum = wv_half[x].astype(F32)
    for d in range(1, NX):
        w_sum += wv_in[d - 1].astype(F32)
    for j in range(NY):
        sums[j] = w_sum[(j // 2) * 16 : (j // 2 + 1) * 16, (j % 2) * 128 : (j % 2 + 1) * 128].astype(BF16)
    y_sum = [remote(sums.at[step(y, d, NY)], sum_in.at[d - 1], y=step(y, d, NY)) for d in range(1, NY)]
    over_z(0, 5)
    over_z(0, 6)
    for copy in c_wkv:
        copy.wait_recv()
    dk_rows = gathered[0].reshape(NZ * 32, 512)
    w_key = wkv[:, :, 0].reshape(NX * 64, 512)
    w_value = wkv[:, :, 1].reshape(NX * 64, 512)
    grad = mm(w_key, dk_rows, NT) + mm(w_value, dv_rows, NT)
    for xx in range(NX):
        dst_part[xx] = grad[xx * 64 : (xx + 1) * 64].astype(BF16)
    x_ds = [remote(dst_part.at[step(x, d, NX)], dst_in.at[x], x=step(x, d, NX)) for d in range(1, NX)]
    dst_in[x] = dst_part[x]
    dq_over_z(5)
    dq_over_z(6)
    for copy in c_wq:
        copy.wait_recv()
    out = jnp.zeros((32, NX * 64), F32)
    for zz in range(NZ):
        cols = slice(zz * HEAD_DIM, (zz + 1) * HEAD_DIM)
        out += mm(dq_all[zz], wq[:, :, :, cols].reshape(NX * 64, HEAD_DIM), NT)
    for half in range(2):
        dtp[half] = out[:, half * 128 : (half + 1) * 128].astype(BF16)
    x_dt = [remote(dtp.at[step(x, d, NX) // 2], dt_in.at[x], x=step(x, d, NX)) for d in range(1, NX)]
    dt_in[x] = dtp[x // 2]
    for copy in y_sum:
        copy.wait_recv()
    own_sum = sums[y].astype(F32)
    for d in range(1, NY):
        own_sum += sum_in[d - 1].astype(F32)
    total[...] = own_sum.astype(BF16)
    sp_all = [
        remote(total, totals.at[y, c], y=step(y, dy, NY), c=lax.rem(c + dc, NC))
        for dy in range(NY)
        for dc in range(NC)
        if dy or dc
    ]
    totals[y, c] = own_sum.astype(BF16)

    for copy in x_ds:
        copy.wait_recv()
    for xx in range(NX):
        ds_rows[:, xx] = jnp.transpose(dst_in[xx].astype(F32)).reshape(NZ, 32, 64)
    for zz in range(NZ):
        ds_ref[:, zz * 128 : (zz + 1) * 128] = jnp.transpose(ds_rows[zz].reshape(128, 64)).astype(BF16)
    for copy in x_dt:
        copy.wait_recv()
    both = jnp.transpose(dt_in[...].reshape(128, 128).astype(F32))
    dt_ref[...] = jnp.where(lax.rem(x, 2) == 1, both[64:], both[:64]).astype(BF16)
    for copy in sp_all:
        copy.wait_recv()
    for j in range(NY):
        for cc in range(NC):
            lanes = slice(cc * 256 + (j % 2) * 128, cc * 256 + (j % 2 + 1) * 128)
            dw_ref[(j // 2) * 16 : (j // 2 + 1) * 16, lanes] = totals[j, cc].astype(F32)
    for copy in made[-SENDS:]:
        copy.wait_send()


def put(dt_ref, ds_ref, dw_ref, dt_out, ds_out, dw_out, sem):
    copies = [
        pltpu.make_async_copy(src, dst, sem.at[n])
        for n, (src, dst) in enumerate(((dt_ref, dt_out), (ds_ref, ds_out), (dw_ref, dw_out)))
    ]
    for copy in copies:
        copy.start()
    for copy in copies:
        copy.wait()


def shards(queries, attn_out, log_norm, cotangent, keys, values, source, w_query, w_key, w_value):
    hbm = pl.BlockSpec(memory_space=pl.ANY)
    vmem = pl.BlockSpec(memory_space=pltpu.VMEM)

    def bf(*shape):
        return pltpu.VMEM(shape, BF16)

    def f32(*shape):
        return pltpu.VMEM(shape, F32)

    d_target, d_source, d_wvalue = pl.pallas_call(
        kernel,
        out_shape=(bf(64, 128), bf(64, 1536), f32(64, 512)),
        in_specs=[hbm] * 10,
        out_specs=(vmem,) * 3,
        scratch_shapes=[
            bf(128, 3072), bf(128, 3072), bf(128, 3072), f32(12, 128), bf(64, 1536),
            bf(NY, NC, 2, 2, 16, 512),
            bf(2, 768, 256), bf(2, 768, 256), f32(2, 1, 768), f32(2, 1, 768), f32(1536, 256),
            bf(NC, NY, 2, 2, 16, 512), bf(NY, 2, 2, 16, 512), bf(NY, 2, 2, 16, 512),
            bf(4, 4, 2, 16, 512), bf(4, 2, 16, 512), bf(2, 2, 16, 512),
            bf(NX, 6, 2, 32, 256), bf(NX - 1, 6, 2, 32, 256), f32(32, 256),
            bf(2, 6, 32, 256), bf(2, 6, 32, 256), bf(32, 256),
            bf(2, NZ, 2, 16, 512), bf(NZ, 32, 256),
            bf(NX, 2, 2, 32, 512), bf(NX, 2, 32, 3072), bf(NX, NZ, 32, 64), bf(NX, NZ, 32, 64),
            bf(2, NX, 64, 256), bf(NX, 64, 256), bf(NX, 64, 256), bf(NX - 1, 64, 256),
            bf(NY, 16, 128), bf(NY - 1, 16, 128), bf(16, 128), bf(NY, NC, 16, 128),
            bf(NX, 64, 384), bf(NX, 64, 384), f32(NZ, NX, 32, 64), bf(2, 32, 128), bf(NX, 32, 128),
            pltpu.SemaphoreType.REGULAR((3, 2)), pltpu.SemaphoreType.DMA((10,)),
            pltpu.SemaphoreType.DMA((SENDS,)), pltpu.SemaphoreType.DMA((COPIES,)),
        ],
        compiler_params=pltpu.CompilerParams(
            collective_id=0, has_side_effects=True, vmem_limit_bytes=56 * 2**20
        ),
    )(
        queries, attn_out, cotangent, jnp.transpose(log_norm),
        keys.reshape(2, 16, 512), values.reshape(2, 16, 512), jnp.transpose(source),
        w_key.reshape(2, 32, 512), w_value.reshape(2, 32, 512), w_query.reshape(2, 32, 3072),
    )
    d_target, d_source, d_wvalue = pl.pallas_call(
        put,
        out_shape=(
            jax.ShapeDtypeStruct((64, 128), BF16),
            jax.ShapeDtypeStruct((64, 1536), BF16),
            jax.ShapeDtypeStruct((64, 512), F32),
        ),
        in_specs=[vmem] * 3,
        out_specs=(hbm,) * 3,
        scratch_shapes=[pltpu.SemaphoreType.DMA((3,))],
    )(*(pltpu.with_memory_space_constraint(a, pltpu.VMEM) for a in (d_target, d_source, d_wvalue)))
    return jnp.transpose(d_target), jnp.transpose(d_source), d_wvalue


def solution(mesh):
    split = Mesh(mesh.devices.reshape(NY, NC, NZ, NX), ("y", "c", "z", "x"))
    sp, tp = ("y", "c"), ("z", "x")
    every = sp + tp
    in_specs = (
        P(sp, None), P(sp, None), P(sp, None), P(sp, None),
        P(every, None), P(every, None), P(sp, tp),
        P(tp, None), P(tp, None), P(tp, None),
    )
    out_specs = (P(sp, tp), P(sp, tp), P(tp, None))
    return jax.shard_map(
        shards, mesh=split, in_specs=in_specs, out_specs=out_specs, check_vma=False
    )
```

```python
import math

import jax
import jax.numpy as jnp
from jax import lax
from jax.experimental import pallas as pl
from jax.experimental.pallas import tpu as pltpu
from jax.sharding import Mesh
from jax.sharding import PartitionSpec as P

HEADS = 12
KV_HEADS = 2
HEAD_DIM = 256
PER_GROUP = HEADS // KV_HEADS
NY, NC, NZ, NX = 8, 2, 12, 4
MESH = pl.DeviceIdType.MESH
F32 = jnp.float32
BF16 = jnp.bfloat16
NT = (((1,), (1,)), ((), ()))
TN = (((0,), (0,)), ((), ()))
NN = (((1,), (0,)), ((), ()))
Y_CHAINS = ((0, 1, 4), (1, -1, 4), (1, 1, 3), (0, -1, 3))
Z_CHAINS = ((0, 1, 6), (1, -1, 6), (1, 1, 5), (0, -1, 5))
DQ_CHAINS = ((None, 1, 6), (None, -1, 5))
Y_JUMP, Z_JUMP = 2, 2
NEAR, FAR = (0, 1, -1, 2), (4, 3, -3, -2)
COPIES, SENDS = 196, 64


def mm(a, b, dims):
    return lax.dot_general(a, b, dims, preferred_element_type=F32)


def kernel(
    q_hbm, o_hbm, do_hbm, lse_hbm, k_hbm, v_hbm, src_hbm, wk_hbm, wv_hbm, wq_hbm,
    dt_ref, ds_ref, dw_ref,
    q_ref, o_ref, do_ref, lse_ref, src_ref,
    kv, qs, dos, delta, lse, dq_acc, part, from_core, paired, ring_in, ring_out, own,
    dqp, x_in, x_sum, z_in, z_out, chunk, gathered, dq_all,
    wkv, wq, sxo, sx, wvp, wv_core, wv_half, wv_in, sums, sum_in, total, totals,
    dst_part, dst_in, ds_rows, dtp, dt_in,
    z_sem, local_sem, send_sem, recv_sem,
):
    y, c, z, x = (lax.axis_index(a) for a in ("y", "c", "z", "x"))
    scale = 1.0 / math.sqrt(HEAD_DIM)
    made = []

    def step(v, d, n):
        return lax.rem(v + d + n, n)

    def remote(src, dst, **where):
        number = len(made)
        if number >= SENDS:
            made[number - SENDS].wait_send()
        copy = pltpu.make_async_remote_copy(
            src_ref=src,
            dst_ref=dst,
            send_sem=send_sem.at[number % SENDS],
            recv_sem=recv_sem.at[number],
            device_id=where,
            device_id_type=MESH,
        )
        copy.start()
        made.append(copy)
        return copy

    def spread(copies, name, axis, here, size, d, length, jump, at, t):
        if t:
            copies[name, t].wait_recv()
        if t % jump == 0:
            for far in range(min(jump, length - t), 0, -1):
                src, dst = at(t)
                copies[name, t + far] = remote(src, dst, **{axis: step(here, d * far, size)})

    here = {}

    def load(name, src, dst):
        here[name] = pltpu.make_async_copy(src, dst, local_sem.at[len(here)])
        here[name].start()

    barrier = pltpu.get_barrier_semaphore()
    peers = [{"y": step(y, d, NY)} for d in (1, -1, 2, -2)] + [{"c": 1 - c}]
    peers += [{"x": step(x, d, NX)} for d in range(1, NX)]
    for peer in peers:
        pl.semaphore_signal(barrier, inc=1, device_id=peer, device_id_type=MESH)
    near_z = [step(z, d, NZ) for d in (1, -1, 2, -2)]
    lower = (z + 1) // NZ + (z - 1 + NZ) // NZ + (z + 2) // NZ + (z - 2 + NZ) // NZ

    def greet(sem, to):
        pl.semaphore_signal(sem, inc=1, device_id={"z": to}, device_id_type=MESH)

    for to in near_z:
        pl.when(to > z)(lambda to=to: greet(barrier, to))
    load("v", v_hbm, kv.at[y, c, :, 1])
    load("k", k_hbm, kv.at[y, c, :, 0])
    load("wk", wk_hbm, wkv.at[x, :, 0])
    load("wv", wv_hbm, wkv.at[x, :, 1])
    load("src", src_hbm, src_ref)
    load("q", q_hbm, q_ref)
    load("do", do_hbm, do_ref)
    load("o", o_hbm, o_ref)
    load("lse", lse_hbm, lse_ref)
    load("wq", wq_hbm, wq.at[x])

    here["k"].wait()
    here["v"].wait()
    pl.semaphore_wait(barrier, len(peers) + lower)
    for to in near_z:
        pl.when(to < z)(lambda to=to: greet(z_sem, to))

    hops = {}
    ways = {}
    core_kv = {}

    def kv_spread(t):
        for r, d, length in Y_CHAINS:
            if t > length:
                continue
            block = kv.at[step(y, -d * t, NY), c, r]
            spread(ways, (r, d), "y", y, NY, d, length, Y_JUMP, lambda t: (block, block), t)
            if t:
                core_kv[4 if t == 4 else -d * t, r] = remote(block, block, c=1 - c)

    kv_spread(0)
    core_kv[0] = remote(kv.at[y, c], kv.at[y, c], c=1 - c)
    here["wk"].wait()
    here["wv"].wait()
    x_wkv = [remote(wkv.at[x, c], wkv.at[x, c], x=step(x, d, NX)) for d in range(1, NX)]
    here["src"].wait()
    for zz in range(NZ):
        rows = jnp.transpose(src_ref[:, zz * 128 : (zz + 1) * 128].astype(F32)).astype(BF16)
        for xx in range(NX):
            sxo[xx, zz] = rows[xx * 32 : (xx + 1) * 32]
    x_src = [remote(sxo.at[step(x, d, NX)], sx.at[x], x=step(x, d, NX)) for d in range(1, NX)]

    for name in ("q", "do", "o", "lse"):
        here[name].wait()

    def prepare(g):
        for h in range(PER_GROUP):
            head = g * PER_GROUP + h
            columns = slice(head * HEAD_DIM, (head + 1) * HEAD_DIM)
            rows = slice(h * 128, (h + 1) * 128)
            qs[g, rows] = q_ref[:, columns]
            dos[g, rows] = do_ref[:, columns]
            prod = do_ref[:, columns].astype(F32) * o_ref[:, columns].astype(F32)
            halves = prod[:, :128] + prod[:, 128:]
            delta[g, :, rows] = jnp.sum(jnp.transpose(halves), axis=0, keepdims=True)
            lse[g, :, rows] = lse_ref[head : head + 1]

    def attend(offsets, first):
        for d in offsets:
            for r in range(2):
                if (d, r) in core_kv:
                    core_kv[d, r].wait_recv()
        if first:
            core_kv[0].wait_recv()
        places = [(d, lax.rem(c + dc, NC)) for d in offsets for dc in range(NC)]
        for g in range(KV_HEADS):
            cols = slice(g * HEAD_DIM, (g + 1) * HEAD_DIM)

            def rows_of(w):
                return jnp.concatenate(
                    [kv[step(y, d, NY), cc, :, w, :, cols].reshape(32, HEAD_DIM) for d, cc in places], axis=0
                )

            kb, vb = rows_of(0), rows_of(1)
            scores = mm(kb, qs[g], NT) * scale
            probs = jnp.exp(scores - lse[g])
            dprob = mm(vb, dos[g], NT)
            dscore = (probs * (dprob - delta[g])).astype(BF16)
            dk = (mm(dscore, qs[g], NN) * scale).astype(BF16)
            dv = mm(probs.astype(BF16), dos[g], NN).astype(BF16)
            term = mm(dscore, kb, TN) * scale
            at = slice(g * 768, (g + 1) * 768)
            dq_acc[at] = term if first else dq_acc[at] + term
            for n, (d, cc) in enumerate(places):
                rows = slice(n * 32, n * 32 + 32)
                part[cc, step(y, d, NY), :, 0, :, cols] = dk[rows].reshape(2, 16, HEAD_DIM)
                part[cc, step(y, d, NY), :, 1, :, cols] = dv[rows].reshape(2, 16, HEAD_DIM)

    core_in = {}

    def to_core(offsets):
        for d in offsets:
            at = step(y, d, NY)
            core_in[d] = remote(part.at[1 - c, at], from_core.at[at], c=1 - c)

    def pair(offsets):
        for d in offsets:
            core_in[d].wait_recv()
            at = step(y, d, NY)
            paired[at] = (part[c, at].astype(F32) + from_core[at].astype(F32)).astype(BF16)

    prepare(0)
    kv_spread(1)
    prepare(1)
    kv_spread(2)
    attend(NEAR, True)
    to_core(NEAR)
    kv_spread(3)
    kv_spread(4)
    pair(NEAR)
    attend(FAR, False)

    to_core(FAR)
    x_dq = {}
    for m in range(6):
        for s, d in enumerate((6 - m, m - 5)):
            for xx in range(NX):
                at = pl.multiple_of(step(z, d, NZ) * 128 + xx * 32, 32)
                dqp[xx, m, s] = dq_acc[pl.ds(at, 32)].astype(BF16)
        for d in range(1, NX):
            x_dq[m, d] = remote(dqp.at[step(x, d, NX), m], x_in.at[d - 1, m], x=step(x, d, NX))
    here["wq"].wait()
    x_wq = [remote(wq.at[x, c], wq.at[x, c], x=step(x, d, NX)) for d in range(1, NX)]

    pair(FAR)
    y_sent = {}

    def y_send(w, n, t, value_ref):
        far = 2 - t % 2
        y_sent[w, n, t] = remote(value_ref, ring_in.at[w, n, t - 1], y=step(y, Y_CHAINS[n][1] * far, NY))

    def y_start(w, distances):
        for t in distances:
            for n, (r, d, length) in enumerate(Y_CHAINS):
                if t <= length:
                    y_send(w, n, t, paired.at[step(y, d * t, NY), r, w])

    for w, distances in ((1, (4, 3)), (0, (4, 3)), (1, (1,)), (0, (1,))):
        y_start(w, distances)

    def y_middle(w):
        for n, (r, d, length) in enumerate(Y_CHAINS):
            rows = paired[step(y, d * 2, NY), r, w].astype(F32)
            for t in range(3, length + 1):
                y_sent[w, n, t].wait_recv()
                rows += ring_in[w, n, t - 1].astype(F32)
            ring_out[w, n] = rows.astype(BF16)
            y_send(w, n, 2, ring_out.at[w, n])

    def y_end(w):
        for r in range(2):
            rows = paired[y, r, w].astype(F32)
            for n, (r_, d, length) in enumerate(Y_CHAINS):
                if r_ == r:
                    for t in (1, 2):
                        y_sent[w, n, t].wait_recv()
                        rows += ring_in[w, n, t - 1].astype(F32)
            own[w, r] = rows.astype(BF16)
        gathered[w, z] = own[w]

    z_sent = {}

    def z_send(d, t, rows):
        s = (1, -1).index(d)
        z_out[s, t - 1] = rows.astype(BF16)
        z_sent[d, t] = remote(z_out.at[s, t - 1], z_in.at[s, t - 1], z=step(z, d * (2 - t % 2), NZ))

    def dq_part(m):
        for d in range(1, NX):
            x_dq[m, d].wait_recv()
        rows = dqp[x, m].astype(F32)
        for d in range(1, NX):
            rows += x_in[d - 1, m].astype(F32)
        for s, offset in enumerate((6 - m, m - 5)):
            d, t = (1, -1)[s], abs(offset)
            if t == 6 or t % 2:
                z_send(d, t, rows[s])
            else:
                x_sum[s, t // 2] = rows[s]

    def z_arrived(d, t):
        z_sent[d, t].wait_recv()
        return z_in[(1, -1).index(d), t - 1].astype(F32)

    def z_middle(t):
        for s, (d, length) in enumerate(((1, 6), (-1, 5))):
            rows = x_sum[s, t // 2]
            for far in (1, 2):
                if t + far <= length:
                    rows += z_arrived(d, t + far)
            z_send(d, t, rows)

    @pl.when(z < NZ - 1)
    def _():
        pl.semaphore_wait(z_sem, 4 - lower)

    dq_part(0)
    y_middle(1)
    y_middle(0)
    for m in range(1, 4):
        dq_part(m)
    y_end(1)

    def over_z(w, t):
        for r, d, length in Z_CHAINS:
            if t > length:
                continue
            at = step(z, -d * t, NZ)
            block = gathered.at[w, at, r]
            src = block if t else own.at[w, r]
            spread(ways, (w, r, d), "z", z, NZ, d, length, Z_JUMP, lambda t: (src, block), t)

    def dq_over_z(t):
        for _, d, length in DQ_CHAINS:
            if t > length:
                continue
            block = dq_all.at[step(z, -d * t, NZ)]
            src = block if t else chunk
            spread(ways, ("dq", d), "z", z, NZ, d, length, Z_JUMP, lambda t: (src, block), t)

    over_z(1, 0)
    y_end(0)
    z_middle(4)
    dq_part(4)
    dq_part(5)
    for d in range(1, NX):
        x_wkv[d - 1].wait_recv()
    c_wkv = [remote(wkv.at[step(x, -d, NX), c], wkv.at[step(x, -d, NX), c], c=1 - c) for d in range(1, NX)]
    for copy in x_src:
        copy.wait_recv()
    sx[x] = sxo[x]
    over_z(1, 1)
    over_z(1, 2)
    z_middle(2)
    over_z(0, 0)
    over_z(1, 3)
    over_z(1, 4)
    dq_rows = x_sum[1, 0]
    for d in (1, -1):
        for t in (1, 2):
            dq_rows += z_arrived(d, t)
    chunk[...] = dq_rows.astype(BF16)
    dq_over_z(0)
    dq_all[z] = chunk[...]
    over_z(0, 1)
    over_z(0, 2)
    over_z(1, 5)
    over_z(1, 6)

    dv_rows = gathered[1].reshape(NZ * 32, 512)
    for xx in range(NX):
        term = mm(sx[xx].reshape(NZ * 32, 64), dv_rows, TN).astype(BF16)
        for half in range(2):
            wvp[half, xx] = term[:, half * 256 : (half + 1) * 256]
    core_wv = remote(wvp.at[1 - c], wv_core, c=1 - c)
    dq_over_z(1)
    dq_over_z(2)
    core_wv.wait_recv()
    wv_half[...] = (wvp[c].astype(F32) + wv_core[...].astype(F32)).astype(BF16)
    x_wv = [remote(wv_half.at[step(x, d, NX)], wv_in.at[d - 1], x=step(x, d, NX)) for d in range(1, NX)]
    over_z(0, 3)
    over_z(0, 4)
    dq_over_z(3)
    dq_over_z(4)
    for d in range(1, NX):
        x_wq[d - 1].wait_recv()
    c_wq = [remote(wq.at[step(x, -d, NX), c], wq.at[step(x, -d, NX), c], c=1 - c) for d in range(1, NX)]
    for copy in x_wv:
        copy.wait_recv()
    w_sum = wv_half[x].astype(F32)
    for d in range(1, NX):
        w_sum += wv_in[d - 1].astype(F32)
    for j in range(NY):
        sums[j] = w_sum[(j // 2) * 16 : (j // 2 + 1) * 16, (j % 2) * 128 : (j % 2 + 1) * 128].astype(BF16)
    y_sum = [remote(sums.at[step(y, d, NY)], sum_in.at[d - 1], y=step(y, d, NY)) for d in range(1, NY)]
    over_z(0, 5)
    over_z(0, 6)
    for copy in c_wkv:
        copy.wait_recv()
    dk_rows = gathered[0].reshape(NZ * 32, 512)
    w_key = wkv[:, :, 0].reshape(NX * 64, 512)
    w_value = wkv[:, :, 1].reshape(NX * 64, 512)
    grad = mm(w_key, dk_rows, NT) + mm(w_value, dv_rows, NT)
    for xx in range(NX):
        dst_part[xx] = grad[xx * 64 : (xx + 1) * 64].astype(BF16)
    x_ds = [remote(dst_part.at[step(x, d, NX)], dst_in.at[x], x=step(x, d, NX)) for d in range(1, NX)]
    dst_in[x] = dst_part[x]
    dq_over_z(5)
    dq_over_z(6)
    for copy in c_wq:
        copy.wait_recv()
    out = jnp.zeros((32, NX * 64), F32)
    for zz in range(NZ):
        cols = slice(zz * HEAD_DIM, (zz + 1) * HEAD_DIM)
        out += mm(dq_all[zz], wq[:, :, :, cols].reshape(NX * 64, HEAD_DIM), NT)
    for half in range(2):
        dtp[half] = out[:, half * 128 : (half + 1) * 128].astype(BF16)
    x_dt = [remote(dtp.at[step(x, d, NX) // 2], dt_in.at[x], x=step(x, d, NX)) for d in range(1, NX)]
    dt_in[x] = dtp[x // 2]
    for copy in y_sum:
        copy.wait_recv()
    own_sum = sums[y].astype(F32)
    for d in range(1, NY):
        own_sum += sum_in[d - 1].astype(F32)
    total[...] = own_sum.astype(BF16)
    sp_all = [
        remote(total, totals.at[y, c], y=step(y, dy, NY), c=lax.rem(c + dc, NC))
        for dy in range(NY)
        for dc in range(NC)
        if dy or dc
    ]
    totals[y, c] = own_sum.astype(BF16)

    for copy in x_ds:
        copy.wait_recv()
    for xx in range(NX):
        ds_rows[:, xx] = jnp.transpose(dst_in[xx].astype(F32)).reshape(NZ, 32, 64)
    for zz in range(NZ):
        ds_ref[:, zz * 128 : (zz + 1) * 128] = jnp.transpose(ds_rows[zz].reshape(128, 64)).astype(BF16)
    for copy in x_dt:
        copy.wait_recv()
    both = jnp.transpose(dt_in[...].reshape(128, 128).astype(F32))
    dt_ref[...] = jnp.where(lax.rem(x, 2) == 1, both[64:], both[:64]).astype(BF16)
    for copy in sp_all:
        copy.wait_recv()
    for j in range(NY):
        for cc in range(NC):
            lanes = slice(cc * 256 + (j % 2) * 128, cc * 256 + (j % 2 + 1) * 128)
            dw_ref[(j // 2) * 16 : (j // 2 + 1) * 16, lanes] = totals[j, cc].astype(F32)
    for copy in made[-SENDS:]:
        copy.wait_send()


def put(dt_ref, ds_ref, dw_ref, dt_out, ds_out, dw_out, sem):
    copies = [
        pltpu.make_async_copy(src, dst, sem.at[n])
        for n, (src, dst) in enumerate(((dt_ref, dt_out), (ds_ref, ds_out), (dw_ref, dw_out)))
    ]
    for copy in copies:
        copy.start()
    for copy in copies:
        copy.wait()


def shards(queries, attn_out, log_norm, cotangent, keys, values, source, w_query, w_key, w_value):
    hbm = pl.BlockSpec(memory_space=pl.ANY)
    vmem = pl.BlockSpec(memory_space=pltpu.VMEM)

    def bf(*shape):
        return pltpu.VMEM(shape, BF16)

    def f32(*shape):
        return pltpu.VMEM(shape, F32)

    d_target, d_source, d_wvalue = pl.pallas_call(
        kernel,
        out_shape=(bf(64, 128), bf(64, 1536), f32(64, 512)),
        in_specs=[hbm] * 10,
        out_specs=(vmem,) * 3,
        scratch_shapes=[
            bf(128, 3072), bf(128, 3072), bf(128, 3072), f32(12, 128), bf(64, 1536),
            bf(NY, NC, 2, 2, 16, 512),
            bf(2, 768, 256), bf(2, 768, 256), f32(2, 1, 768), f32(2, 1, 768), f32(1536, 256),
            bf(NC, NY, 2, 2, 16, 512), bf(NY, 2, 2, 16, 512), bf(NY, 2, 2, 16, 512),
            bf(2, 4, 4, 16, 512), bf(2, 4, 16, 512), bf(2, 2, 16, 512),
            bf(NX, 6, 2, 32, 256), bf(NX - 1, 6, 2, 32, 256), f32(2, 3, 32, 256),
            bf(2, 6, 32, 256), bf(2, 6, 32, 256), bf(32, 256),
            bf(2, NZ, 2, 16, 512), bf(NZ, 32, 256),
            bf(NX, 2, 2, 32, 512), bf(NX, 2, 32, 3072), bf(NX, NZ, 32, 64), bf(NX, NZ, 32, 64),
            bf(2, NX, 64, 256), bf(NX, 64, 256), bf(NX, 64, 256), bf(NX - 1, 64, 256),
            bf(NY, 16, 128), bf(NY - 1, 16, 128), bf(16, 128), bf(NY, NC, 16, 128),
            bf(NX, 64, 384), bf(NX, 64, 384), f32(NZ, NX, 32, 64), bf(2, 32, 128), bf(NX, 32, 128),
            pltpu.SemaphoreType.REGULAR, pltpu.SemaphoreType.DMA((10,)),
            pltpu.SemaphoreType.DMA((SENDS,)), pltpu.SemaphoreType.DMA((COPIES,)),
        ],
        compiler_params=pltpu.CompilerParams(
            collective_id=0, has_side_effects=True, vmem_limit_bytes=56 * 2**20
        ),
    )(
        queries, attn_out, cotangent, jnp.transpose(log_norm),
        keys.reshape(2, 16, 512), values.reshape(2, 16, 512), jnp.transpose(source),
        w_key.reshape(2, 32, 512), w_value.reshape(2, 32, 512), w_query.reshape(2, 32, 3072),
    )
    d_target, d_source, d_wvalue = pl.pallas_call(
        put,
        out_shape=(
            jax.ShapeDtypeStruct((64, 128), BF16),
            jax.ShapeDtypeStruct((64, 1536), BF16),
            jax.ShapeDtypeStruct((64, 512), F32),
        ),
        in_specs=[vmem] * 3,
        out_specs=(hbm,) * 3,
        scratch_shapes=[pltpu.SemaphoreType.DMA((3,))],
    )(*(pltpu.with_memory_space_constraint(a, pltpu.VMEM) for a in (d_target, d_source, d_wvalue)))
    return jnp.transpose(d_target), jnp.transpose(d_source), d_wvalue


def solution(mesh):
    split = Mesh(mesh.devices.reshape(NY, NC, NZ, NX), ("y", "c", "z", "x"))
    sp, tp = ("y", "c"), ("z", "x")
    every = sp + tp
    in_specs = (
        P(sp, None), P(sp, None), P(sp, None), P(sp, None),
        P(every, None), P(every, None), P(sp, tp),
        P(tp, None), P(tp, None), P(tp, None),
    )
    out_specs = (P(sp, tp), P(sp, tp), P(tp, None))
    return jax.shard_map(
        shards, mesh=split, in_specs=in_specs, out_specs=out_specs, check_vma=False
    )
```

```python
import math

import jax
import jax.numpy as jnp
from jax import lax
from jax.experimental import pallas as pl
from jax.experimental.pallas import tpu as pltpu
from jax.sharding import Mesh
from jax.sharding import PartitionSpec as P

HEADS = 12
KV_HEADS = 2
HEAD_DIM = 256
PER_GROUP = HEADS // KV_HEADS
NY, NC, NZ, NX = 8, 2, 12, 4
MESH = pl.DeviceIdType.MESH
F32 = jnp.float32
BF16 = jnp.bfloat16
NT = (((1,), (1,)), ((), ()))
TN = (((0,), (0,)), ((), ()))
NN = (((1,), (0,)), ((), ()))
Y_CHAINS = ((0, 1, 4), (1, -1, 4), (1, 1, 3), (0, -1, 3))
Z_CHAINS = ((0, 1, 6), (1, -1, 6), (1, 1, 5), (0, -1, 5))
DQ_CHAINS = ((None, 1, 6), (None, -1, 5))
Y_JUMP, Z_JUMP = 2, 2
NEAR, FAR = (0, 1, -1, 2), (4, 3, -3, -2)
COPIES, SENDS = 158, 64


def mm(a, b, dims):
    return lax.dot_general(a, b, dims, preferred_element_type=F32)


def kernel(
    q_hbm, o_hbm, do_hbm, lse_hbm, k_hbm, v_hbm, src_hbm, wk_hbm, wv_hbm, wq_hbm,
    dt_ref, ds_ref, dw_ref,
    q_ref, o_ref, do_ref, lse_ref, src_ref,
    kv, qs, dos, delta, lse, dq_acc, part, from_core, paired, ring_in, ring_out, own,
    dqp, x_in, x_sum, z_in, z_out, chunk, gathered, dq_all,
    wkv, wq, sxo, sx, wvp, wv_core, wv_half, wv_in, sums, sum_in, total, totals,
    dst_part, dst_in, ds_rows, dtp, dt_in,
    z_sem, local_sem, send_sem, recv_sem,
):
    y, c, z, x = (lax.axis_index(a) for a in ("y", "c", "z", "x"))
    scale = 1.0 / math.sqrt(HEAD_DIM)
    made, places, groups = [], [], {}

    def step(v, d, n):
        return lax.rem(v + d + n, n)

    def remote(src, dst, group=None, **where):
        number = len(made)
        place = groups.get(group)
        if place is None:
            place = len(places)
            places.append(group)
            if group is not None:
                groups[group] = place
        if number >= SENDS:
            made[number - SENDS].wait_send()
        copy = pltpu.make_async_remote_copy(
            src_ref=src,
            dst_ref=dst,
            send_sem=send_sem.at[number % SENDS],
            recv_sem=recv_sem.at[place],
            device_id=where,
            device_id_type=MESH,
        )
        copy.start()
        made.append(copy)
        return copy

    def spread(copies, name, axis, here, size, d, length, jump, at, t):
        if t:
            copies[name, t].wait_recv()
        if t % jump == 0:
            for far in range(min(jump, length - t), 0, -1):
                src, dst = at(t)
                copies[name, t + far] = remote(src, dst, **{axis: step(here, d * far, size)})

    def take(group, whole):
        pltpu.make_async_copy(whole, whole, recv_sem.at[groups[group]]).wait()

    here = {}

    def load(name, src, dst):
        here[name] = pltpu.make_async_copy(src, dst, local_sem.at[len(here)])
        here[name].start()

    barrier = pltpu.get_barrier_semaphore()
    peers = [{"y": step(y, d, NY)} for d in (1, -1, 2, -2)] + [{"c": 1 - c}]
    peers += [{"x": step(x, d, NX)} for d in range(1, NX)]
    for peer in peers:
        pl.semaphore_signal(barrier, inc=1, device_id=peer, device_id_type=MESH)
    near_z = [step(z, d, NZ) for d in (1, -1, 2, -2)]
    lower = (z + 1) // NZ + (z - 1 + NZ) // NZ + (z + 2) // NZ + (z - 2 + NZ) // NZ

    def greet(sem, to):
        pl.semaphore_signal(sem, inc=1, device_id={"z": to}, device_id_type=MESH)

    for to in near_z:
        pl.when(to > z)(lambda to=to: greet(barrier, to))
    load("v", v_hbm, kv.at[y, c, :, 1])
    load("k", k_hbm, kv.at[y, c, :, 0])
    load("wk", wk_hbm, wkv.at[x, :, 0])
    load("wv", wv_hbm, wkv.at[x, :, 1])
    load("src", src_hbm, src_ref)
    load("q", q_hbm, q_ref)
    load("do", do_hbm, do_ref)
    load("o", o_hbm, o_ref)
    load("lse", lse_hbm, lse_ref)
    load("wq", wq_hbm, wq.at[x])

    here["k"].wait()
    here["v"].wait()
    pl.semaphore_wait(barrier, len(peers) + lower)
    for to in near_z:
        pl.when(to < z)(lambda to=to: greet(z_sem, to))

    hops = {}
    ways = {}
    core_kv = {}

    def kv_spread(t):
        for r, d, length in Y_CHAINS:
            if t > length:
                continue
            block = kv.at[step(y, -d * t, NY), c, r]
            spread(ways, (r, d), "y", y, NY, d, length, Y_JUMP, lambda t: (block, block), t)
            if t:
                core_kv[4 if t == 4 else -d * t, r] = remote(block, block, c=1 - c)

    kv_spread(0)
    core_kv[0] = remote(kv.at[y, c], kv.at[y, c], c=1 - c)
    here["wk"].wait()
    here["wv"].wait()
    x_wkv = [remote(wkv.at[x, c], wkv.at[x, c], x=step(x, d, NX)) for d in range(1, NX)]
    here["src"].wait()
    for zz in range(NZ):
        rows = jnp.transpose(src_ref[:, zz * 128 : (zz + 1) * 128].astype(F32)).astype(BF16)
        for xx in range(NX):
            sxo[xx, zz] = rows[xx * 32 : (xx + 1) * 32]
    x_src = [remote(sxo.at[step(x, d, NX)], sx.at[x], x=step(x, d, NX)) for d in range(1, NX)]

    for name in ("q", "do", "o", "lse"):
        here[name].wait()

    def prepare(g):
        for h in range(PER_GROUP):
            head = g * PER_GROUP + h
            columns = slice(head * HEAD_DIM, (head + 1) * HEAD_DIM)
            rows = slice(h * 128, (h + 1) * 128)
            qs[g, rows] = q_ref[:, columns]
            dos[g, rows] = do_ref[:, columns]
            prod = do_ref[:, columns].astype(F32) * o_ref[:, columns].astype(F32)
            halves = prod[:, :128] + prod[:, 128:]
            delta[g, :, rows] = jnp.sum(jnp.transpose(halves), axis=0, keepdims=True)
            lse[g, :, rows] = lse_ref[head : head + 1]

    def attend(offsets, first):
        for d in offsets:
            for r in range(2):
                if (d, r) in core_kv:
                    core_kv[d, r].wait_recv()
        if first:
            core_kv[0].wait_recv()
        places = [(d, lax.rem(c + dc, NC)) for d in offsets for dc in range(NC)]
        for g in range(KV_HEADS):
            cols = slice(g * HEAD_DIM, (g + 1) * HEAD_DIM)

            def rows_of(w):
                return jnp.concatenate(
                    [kv[step(y, d, NY), cc, :, w, :, cols].reshape(32, HEAD_DIM) for d, cc in places], axis=0
                )

            kb, vb = rows_of(0), rows_of(1)
            scores = mm(kb, qs[g], NT) * scale
            probs = jnp.exp(scores - lse[g])
            dprob = mm(vb, dos[g], NT)
            dscore = (probs * (dprob - delta[g])).astype(BF16)
            dk = (mm(dscore, qs[g], NN) * scale).astype(BF16)
            dv = mm(probs.astype(BF16), dos[g], NN).astype(BF16)
            term = mm(dscore, kb, TN) * scale
            at = slice(g * 768, (g + 1) * 768)
            dq_acc[at] = term if first else dq_acc[at] + term
            for n, (d, cc) in enumerate(places):
                rows = slice(n * 32, n * 32 + 32)
                part[cc, step(y, d, NY), :, 0, :, cols] = dk[rows].reshape(2, 16, HEAD_DIM)
                part[cc, step(y, d, NY), :, 1, :, cols] = dv[rows].reshape(2, 16, HEAD_DIM)

    core_in = {}

    def to_core(offsets):
        for d in offsets:
            at = step(y, d, NY)
            core_in[d] = remote(part.at[1 - c, at], from_core.at[at], c=1 - c)

    def pair(offsets):
        for d in offsets:
            core_in[d].wait_recv()
            at = step(y, d, NY)
            paired[at] = (part[c, at].astype(F32) + from_core[at].astype(F32)).astype(BF16)

    prepare(0)
    kv_spread(1)
    prepare(1)
    kv_spread(2)
    attend(NEAR, True)
    to_core(NEAR)
    kv_spread(3)
    kv_spread(4)
    pair(NEAR)
    attend(FAR, False)

    to_core(FAR)
    for m in range(6):
        for s, d in enumerate((6 - m, m - 5)):
            for xx in range(NX):
                at = pl.multiple_of(step(z, d, NZ) * 128 + xx * 32, 32)
                dqp[xx, m, s] = dq_acc[pl.ds(at, 32)].astype(BF16)
        for d in range(1, NX):
            remote(dqp.at[step(x, d, NX), m], x_in.at[m, d - 1], ("x_dq", m), x=step(x, d, NX))
    here["wq"].wait()
    x_wq = [remote(wq.at[x, c], wq.at[x, c], x=step(x, d, NX)) for d in range(1, NX)]

    pair(FAR)
    y_sent = {}

    def y_send(w, n, t, value_ref):
        far = 2 - t % 2
        y_sent[w, n, t] = remote(value_ref, ring_in.at[w, n, t - 1], y=step(y, Y_CHAINS[n][1] * far, NY))

    def y_start(w, distances):
        for t in distances:
            for n, (r, d, length) in enumerate(Y_CHAINS):
                if t <= length:
                    y_send(w, n, t, paired.at[step(y, d * t, NY), r, w])

    for w, distances in ((1, (4, 3)), (0, (4, 3)), (1, (1,)), (0, (1,))):
        y_start(w, distances)

    def y_middle(w):
        for n, (r, d, length) in enumerate(Y_CHAINS):
            rows = paired[step(y, d * 2, NY), r, w].astype(F32)
            for t in range(3, length + 1):
                y_sent[w, n, t].wait_recv()
                rows += ring_in[w, n, t - 1].astype(F32)
            ring_out[w, n] = rows.astype(BF16)
            y_send(w, n, 2, ring_out.at[w, n])

    def y_end(w):
        for r in range(2):
            rows = paired[y, r, w].astype(F32)
            for n, (r_, d, length) in enumerate(Y_CHAINS):
                if r_ == r:
                    for t in (1, 2):
                        y_sent[w, n, t].wait_recv()
                        rows += ring_in[w, n, t - 1].astype(F32)
            own[w, r] = rows.astype(BF16)
        gathered[w, z] = own[w]

    z_sent = {}

    def z_send(d, t, rows):
        s = (1, -1).index(d)
        z_out[s, t - 1] = rows.astype(BF16)
        z_sent[d, t] = remote(z_out.at[s, t - 1], z_in.at[s, t - 1], z=step(z, d * (2 - t % 2), NZ))

    def dq_part(m):
        take(("x_dq", m), x_in.at[m])
        rows = dqp[x, m].astype(F32)
        for d in range(1, NX):
            rows += x_in[m, d - 1].astype(F32)
        for s, offset in enumerate((6 - m, m - 5)):
            d, t = (1, -1)[s], abs(offset)
            if t == 6 or t % 2:
                z_send(d, t, rows[s])
            else:
                x_sum[s, t // 2] = rows[s]

    def z_arrived(d, t):
        z_sent[d, t].wait_recv()
        return z_in[(1, -1).index(d), t - 1].astype(F32)

    def z_middle(t):
        for s, (d, length) in enumerate(((1, 6), (-1, 5))):
            rows = x_sum[s, t // 2]
            for far in (1, 2):
                if t + far <= length:
                    rows += z_arrived(d, t + far)
            z_send(d, t, rows)

    @pl.when(z < NZ - 1)
    def _():
        pl.semaphore_wait(z_sem, 4 - lower)

    dq_part(0)
    y_middle(1)
    y_middle(0)
    for m in range(1, 4):
        dq_part(m)
    y_end(1)

    def over_z(w, t):
        for r, d, length in Z_CHAINS:
            if t > length:
                continue
            at = step(z, -d * t, NZ)
            block = gathered.at[w, at, r]
            src = block if t else own.at[w, r]
            spread(ways, (w, r, d), "z", z, NZ, d, length, Z_JUMP, lambda t: (src, block), t)

    def dq_over_z(t):
        for _, d, length in DQ_CHAINS:
            if t > length:
                continue
            block = dq_all.at[step(z, -d * t, NZ)]
            src = block if t else chunk
            spread(ways, ("dq", d), "z", z, NZ, d, length, Z_JUMP, lambda t: (src, block), t)

    over_z(1, 0)
    y_end(0)
    z_middle(4)
    dq_part(4)
    dq_part(5)
    for d in range(1, NX):
        x_wkv[d - 1].wait_recv()
    c_wkv = [remote(wkv.at[step(x, -d, NX), c], wkv.at[step(x, -d, NX), c], c=1 - c) for d in range(1, NX)]
    for copy in x_src:
        copy.wait_recv()
    sx[x] = sxo[x]
    over_z(1, 1)
    over_z(1, 2)
    z_middle(2)
    over_z(0, 0)
    over_z(1, 3)
    over_z(1, 4)
    dq_rows = x_sum[1, 0]
    for d in (1, -1):
        for t in (1, 2):
            dq_rows += z_arrived(d, t)
    chunk[...] = dq_rows.astype(BF16)
    dq_over_z(0)
    dq_all[z] = chunk[...]
    over_z(0, 1)
    over_z(0, 2)
    over_z(1, 5)
    over_z(1, 6)

    dv_rows = gathered[1].reshape(NZ * 32, 512)
    for xx in range(NX):
        term = mm(sx[xx].reshape(NZ * 32, 64), dv_rows, TN).astype(BF16)
        for half in range(2):
            wvp[half, xx] = term[:, half * 256 : (half + 1) * 256]
    core_wv = remote(wvp.at[1 - c], wv_core, c=1 - c)
    dq_over_z(1)
    dq_over_z(2)
    core_wv.wait_recv()
    wv_half[...] = (wvp[c].astype(F32) + wv_core[...].astype(F32)).astype(BF16)
    [remote(wv_half.at[step(x, d, NX)], wv_in.at[d - 1], "x_wv", x=step(x, d, NX)) for d in range(1, NX)]
    over_z(0, 3)
    over_z(0, 4)
    dq_over_z(3)
    dq_over_z(4)
    for d in range(1, NX):
        x_wq[d - 1].wait_recv()
    c_wq = [remote(wq.at[step(x, -d, NX), c], wq.at[step(x, -d, NX), c], c=1 - c) for d in range(1, NX)]
    take("x_wv", wv_in)
    w_sum = wv_half[x].astype(F32)
    for d in range(1, NX):
        w_sum += wv_in[d - 1].astype(F32)
    for j in range(NY):
        sums[j] = w_sum[(j // 2) * 16 : (j // 2 + 1) * 16, (j % 2) * 128 : (j % 2 + 1) * 128].astype(BF16)
    [remote(sums.at[step(y, d, NY)], sum_in.at[d - 1], "y_sum", y=step(y, d, NY)) for d in range(1, NY)]
    over_z(0, 5)
    over_z(0, 6)
    for copy in c_wkv:
        copy.wait_recv()
    dk_rows = gathered[0].reshape(NZ * 32, 512)
    w_key = wkv[:, :, 0].reshape(NX * 64, 512)
    w_value = wkv[:, :, 1].reshape(NX * 64, 512)
    grad = mm(w_key, dk_rows, NT) + mm(w_value, dv_rows, NT)
    for xx in range(NX):
        dst_part[xx] = grad[xx * 64 : (xx + 1) * 64].astype(BF16)
    [remote(dst_part.at[step(x, d, NX)], dst_in.at[x], "x_ds", x=step(x, d, NX)) for d in range(1, NX)]
    dst_in[x] = dst_part[x]
    dq_over_z(5)
    dq_over_z(6)
    for copy in c_wq:
        copy.wait_recv()
    out = jnp.zeros((32, NX * 64), F32)
    for zz in range(NZ):
        cols = slice(zz * HEAD_DIM, (zz + 1) * HEAD_DIM)
        out += mm(dq_all[zz], wq[:, :, :, cols].reshape(NX * 64, HEAD_DIM), NT)
    for half in range(2):
        dtp[half] = out[:, half * 128 : (half + 1) * 128].astype(BF16)
    [remote(dtp.at[step(x, d, NX) // 2], dt_in.at[x], "x_dt", x=step(x, d, NX)) for d in range(1, NX)]
    dt_in[x] = dtp[x // 2]
    take("y_sum", sum_in)
    own_sum = sums[y].astype(F32)
    for d in range(1, NY):
        own_sum += sum_in[d - 1].astype(F32)
    total[...] = own_sum.astype(BF16)
    [
        remote(total, totals.at[y * NC + c], "sp_all", y=step(y, dy, NY), c=lax.rem(c + dc, NC))
        for dy in range(NY)
        for dc in range(NC)
        if dy or dc
    ]
    totals[y * NC + c] = own_sum.astype(BF16)

    take("x_ds", dst_in.at[pl.ds(0, NX - 1)])
    for xx in range(NX):
        ds_rows[:, xx] = jnp.transpose(dst_in[xx].astype(F32)).reshape(NZ, 32, 64)
    for zz in range(NZ):
        ds_ref[:, zz * 128 : (zz + 1) * 128] = jnp.transpose(ds_rows[zz].reshape(128, 64)).astype(BF16)
    take("x_dt", dt_in.at[pl.ds(0, NX - 1)])
    both = jnp.transpose(dt_in[...].reshape(128, 128).astype(F32))
    dt_ref[...] = jnp.where(lax.rem(x, 2) == 1, both[64:], both[:64]).astype(BF16)
    take("sp_all", totals.at[pl.ds(0, NY * NC - 1)])
    for j in range(NY):
        for cc in range(NC):
            lanes = slice(cc * 256 + (j % 2) * 128, cc * 256 + (j % 2 + 1) * 128)
            dw_ref[(j // 2) * 16 : (j // 2 + 1) * 16, lanes] = totals[j * NC + cc].astype(F32)
    for copy in made[-SENDS:]:
        copy.wait_send()


def put(dt_ref, ds_ref, dw_ref, dt_out, ds_out, dw_out, sem):
    copies = [
        pltpu.make_async_copy(src, dst, sem.at[n])
        for n, (src, dst) in enumerate(((dt_ref, dt_out), (ds_ref, ds_out), (dw_ref, dw_out)))
    ]
    for copy in copies:
        copy.start()
    for copy in copies:
        copy.wait()


def shards(queries, attn_out, log_norm, cotangent, keys, values, source, w_query, w_key, w_value):
    hbm = pl.BlockSpec(memory_space=pl.ANY)
    vmem = pl.BlockSpec(memory_space=pltpu.VMEM)

    def bf(*shape):
        return pltpu.VMEM(shape, BF16)

    def f32(*shape):
        return pltpu.VMEM(shape, F32)

    d_target, d_source, d_wvalue = pl.pallas_call(
        kernel,
        out_shape=(bf(64, 128), bf(64, 1536), f32(64, 512)),
        in_specs=[hbm] * 10,
        out_specs=(vmem,) * 3,
        scratch_shapes=[
            bf(128, 3072), bf(128, 3072), bf(128, 3072), f32(12, 128), bf(64, 1536),
            bf(NY, NC, 2, 2, 16, 512),
            bf(2, 768, 256), bf(2, 768, 256), f32(2, 1, 768), f32(2, 1, 768), f32(1536, 256),
            bf(NC, NY, 2, 2, 16, 512), bf(NY, 2, 2, 16, 512), bf(NY, 2, 2, 16, 512),
            bf(2, 4, 4, 16, 512), bf(2, 4, 16, 512), bf(2, 2, 16, 512),
            bf(NX, 6, 2, 32, 256), bf(6, NX - 1, 2, 32, 256), f32(2, 3, 32, 256),
            bf(2, 6, 32, 256), bf(2, 6, 32, 256), bf(32, 256),
            bf(2, NZ, 2, 16, 512), bf(NZ, 32, 256),
            bf(NX, 2, 2, 32, 512), bf(NX, 2, 32, 3072), bf(NX, NZ, 32, 64), bf(NX, NZ, 32, 64),
            bf(2, NX, 64, 256), bf(NX, 64, 256), bf(NX, 64, 256), bf(NX - 1, 64, 256),
            bf(NY, 16, 128), bf(NY - 1, 16, 128), bf(16, 128), bf(NY * NC, 16, 128),
            bf(NX, 64, 384), bf(NX, 64, 384), f32(NZ, NX, 32, 64), bf(2, 32, 128), bf(NX, 32, 128),
            pltpu.SemaphoreType.REGULAR, pltpu.SemaphoreType.DMA((10,)),
            pltpu.SemaphoreType.DMA((SENDS,)), pltpu.SemaphoreType.DMA((COPIES,)),
        ],
        compiler_params=pltpu.CompilerParams(
            collective_id=0, has_side_effects=True, vmem_limit_bytes=56 * 2**20
        ),
    )(
        queries, attn_out, cotangent, jnp.transpose(log_norm),
        keys.reshape(2, 16, 512), values.reshape(2, 16, 512), jnp.transpose(source),
        w_key.reshape(2, 32, 512), w_value.reshape(2, 32, 512), w_query.reshape(2, 32, 3072),
    )
    d_target, d_source, d_wvalue = pl.pallas_call(
        put,
        out_shape=(
            jax.ShapeDtypeStruct((64, 128), BF16),
            jax.ShapeDtypeStruct((64, 1536), BF16),
            jax.ShapeDtypeStruct((64, 512), F32),
        ),
        in_specs=[vmem] * 3,
        out_specs=(hbm,) * 3,
        scratch_shapes=[pltpu.SemaphoreType.DMA((3,))],
    )(*(pltpu.with_memory_space_constraint(a, pltpu.VMEM) for a in (d_target, d_source, d_wvalue)))
    return jnp.transpose(d_target), jnp.transpose(d_source), d_wvalue


def solution(mesh):
    split = Mesh(mesh.devices.reshape(NY, NC, NZ, NX), ("y", "c", "z", "x"))
    sp, tp = ("y", "c"), ("z", "x")
    every = sp + tp
    in_specs = (
        P(sp, None), P(sp, None), P(sp, None), P(sp, None),
        P(every, None), P(every, None), P(sp, tp),
        P(tp, None), P(tp, None), P(tp, None),
    )
    out_specs = (P(sp, tp), P(sp, tp), P(tp, None))
    return jax.shard_map(
        shards, mesh=split, in_specs=in_specs, out_specs=out_specs, check_vma=False
    )
```
